32 devices in a mesh: ep: 8 (over z, x), tp: 4 (over y, core).
Axes of the slice: x: 2, y: 2, z: 4, core: 2. Of those that a mesh axis runs over, the one named last changes fastest.
Arguments:
- mixer_rows: bfloat16 [1024, 2048], P('ep'), may hold values from -40 to 40
- mixer_gain: float32 [2048], replicated, may hold values from 0.1 to 1.9
- inner_weight: bfloat16 [2048, 1024], P(None, 'tp'), may hold values from -0.125 to 0.125
- gate_in_weight: bfloat16 [2048, 1024], P(None, 'tp'), may hold values from -0.125 to 0.125
- gate_out_weight: bfloat16 [2048, 1024], P(None, 'tp'), may hold values from -0.125 to 0.125
- conv_taps: float32 [3, 1024], P(None, 'tp'), may hold values from -3.5 to 3.5
- mixer_out_weight: bfloat16 [1024, 2048], P('tp'), may hold values from -0.1875 to 0.1875
- routed_rows: bfloat16 [2048, 2048], P('ep'), may hold values from -40 to 40
- routed_gain: float32 [2048], replicated, may hold values from 0.1 to 1.9
- route_ids: int32 [2048, 2], P('ep'), may hold values from 0 to 7, all different within a row; in each aligned block of 256 rows (0 to 255, 256 to 511, ...) at most 128 rows name the same one
- route_weights: float32 [2048, 2], P('ep'), may hold values from 0.25 to 1
- expert_gate: bfloat16 [8, 2048, 2048], P('ep', None, 'tp'), may hold values from -0.125 to 0.125
- expert_up: bfloat16 [8, 2048, 2048], P('ep', None, 'tp'), may hold values from -0.125 to 0.125
- expert_down: bfloat16 [8, 2048, 2048], P('ep', 'tp'), may hold values from -0.125 to 0.125
Outputs:
- mixer_output: bfloat16 [1024, 2048], P('ep')
- routed_output: bfloat16 [2048, 2048], P('ep')
The draws below stay inside these ranges and needn't reach their ends.
Inputs may be any that keep to these rules, and one draw needn't show every extreme that they name: `route_ids`: within each aligned block of 256 tokens, no expert is named by more than 128 choices, a bound that some block reaches; a token's 2 experts differ.
All inputs are finite; a program needn't handle non-finite values.
Results may differ from the reference program's by a relative error of at most 0.019.
Values may be sent and summed in bfloat16 or wider, within the bound.
A program may use at most 64 MiB of HBM per device.

```python
import math
import jax
import jax.numpy as jnp
import numpy as np
from jax import lax

D = 2048
CONV = 1024
TAPS = 3
FF = 2048
TOPK = 2
EXPERTS = 8
TOK2 = 256
TOKENS1 = 1024
TOKENS2 = 2048
CAP = 128
N_TP = 4


def scaled_rows(key, row_total, model_width):
    keys = jax.random.split(key, 3)
    row_scale = jnp.exp(jax.random.uniform(keys[0], (row_total, 1), jnp.float32) * math.log(10.0))
    col_scale = jnp.exp(jax.random.uniform(keys[1], (1, model_width), jnp.float32) * math.log(10.0))
    base = jnp.clip(jax.random.normal(keys[2], (row_total, model_width), jnp.float32), -4.0, 4.0)
    return (base * row_scale * col_scale * 0.1).astype(jnp.bfloat16)


def draw_mixer_rows(key, part):
    return scaled_rows(jax.random.fold_in(key, 11), TOKENS1, D)


def draw_routed_rows(key, part):
    return scaled_rows(jax.random.fold_in(key, 23), TOKENS2, D)


def steps_of(stream_key, shape, pieces, least, top_value):
    loudness, own = 1.0, jax.random.fold_in(stream_key, 6)
    for dim, blocks in pieces:
        steps = jnp.exp(jax.random.uniform(jax.random.fold_in(own, dim), (blocks,), jnp.float32, least / len(pieces), top_value / len(pieces)))
        loudness = loudness * jnp.repeat(steps, shape[dim] // blocks).reshape([-1 if axis == dim else 1 for axis in range(len(shape))])
    return loudness


def assign_block(stream_key, own, number, rows, count, top, most, lean):
    order = jax.random.permutation(stream_key, count)
    crowded, usual = load_shares(count, rows * top, most, lean, True), load_shares(count, rows * top, most, lean, False)
    places = jnp.arange(count)

    def named(sizes, turn):
        used = int((sizes > 0).sum())
        fixed = max(1, used // 4)
        passed = fixed + (places - fixed + turn * (used - fixed)) % max(1, count - fixed)
        return jnp.zeros((count,), jnp.int32).at[order[jnp.where(places < fixed, places, passed)]].set(jnp.asarray(sizes, jnp.int32))

    sizes = jnp.where(number % 4 == 0, named(crowded, number // 4), named(usual, number - number // 4 - 1))
    mixed = jax.random.permutation(jax.random.fold_in(own, 3), count)
    donor, taker = mixed[0:count // 2 * 2:2], mixed[1:count // 2 * 2:2]
    room = jnp.minimum(sizes[donor] - 1, most - sizes[taker]) // 2
    room = jnp.where((donor == order[0]) | (taker == order[0]) | (sizes[taker] == 0), 0, jnp.maximum(room, 0))
    passed = jax.random.randint(jax.random.fold_in(own, 4), (count // 2,), 0, 1 << 20) % (room + 1)
    sizes = sizes.at[donor].add(-passed).at[taker].add(passed)
    members = jnp.searchsorted(jnp.cumsum(sizes), jnp.arange(rows * top), side="right").astype(jnp.int32)
    listing = members.reshape(top, rows).T
    listing = listing[jax.random.permutation(jax.random.fold_in(own, 1), rows)]
    turn = jax.random.randint(jax.random.fold_in(own, 2), (rows, 1), 0, top)
    return jnp.take_along_axis(listing, (jnp.arange(top)[None, :] + turn) % top, axis=1)


def load_shares(number_of, total, limit, skew, full):
    loads = [(1 << 20) // math.isqrt(grade ** skew) + 1 for grade in range(1, number_of + 1)]
    largest = limit if full else min(limit, max(-(-total // number_of), total * loads[0] // sum(loads)))
    least = 1 if total - largest >= number_of - 1 else 0
    given, surplus = [largest] + [least] * (number_of - 1), total - largest - least * (number_of - 1)
    while surplus > 0:
        movable = [i for i in range(1, number_of) if given[i] < largest] or [i for i in range(1, number_of) if given[i] < limit]
        mass, left = sum([loads[i] for i in movable]), surplus
        for i in movable:
            extra = min(limit - given[i], max(1, left * loads[i] // mass), surplus)
            given[i] = given[i] + extra
            surplus = surplus - extra
    return np.array(given)


def noise(key, dims, scale, bound, cuts=(), kind=jnp.bfloat16):
    loudness = steps_of(key, dims, cuts, -0.22, 0.18) if cuts else 1.0
    entries = jax.random.normal(key, dims, jnp.float32) * scale * loudness
    return jnp.minimum(jnp.maximum(entries, -bound), bound).astype(kind)


def setup_inputs(seed: int = 0) -> dict:
    arg_keys = jax.random.split(jax.random.key(seed), 15)
    mixer_rows = draw_mixer_rows(jax.random.fold_in(arg_keys[14], 71), 0)
    mixer_gain = jnp.clip(1.0 + 0.18 * jax.random.normal(arg_keys[1], (D,), jnp.float32), 0.1, 1.9)
    inner_weight = noise(arg_keys[2], (D, CONV), D ** -0.5, 0.125, ((1, 4),))
    gate_in_weight = noise(arg_keys[3], (D, CONV), D ** -0.5, 0.125, ((1, 4),))
    gate_out_weight = noise(arg_keys[4], (D, CONV), D ** -0.5, 0.125, ((1, 4),))
    conv_taps = noise(arg_keys[5], (TAPS, CONV), TAPS ** -0.5, 3.5, ((1, 4),), jnp.float32)
    mixer_out_weight = noise(arg_keys[6], (CONV, D), CONV ** -0.5, 0.1875, ((0, 4),))
    routed_rows = draw_routed_rows(jax.random.fold_in(arg_keys[14], 71), 0)
    routed_gain = jnp.clip(1.0 + 0.18 * jax.random.normal(arg_keys[8], (D,), jnp.float32), 0.1, 1.9)
    route_ids_keys = jax.random.split(jax.random.fold_in(arg_keys[9], 1), TOKENS2 // TOK2)
    route_ids_turns = jax.random.permutation(jax.random.fold_in(arg_keys[9], 3), TOKENS2 // TOK2)
    route_ids = jax.vmap(lambda own, number: assign_block(jax.random.fold_in(arg_keys[9], 2), own, number, TOK2, EXPERTS, TOPK, CAP, 2))(route_ids_keys, route_ids_turns).reshape((TOKENS2, TOPK))
    route_weights = jnp.clip(0.25 + 0.75 * jax.random.uniform(arg_keys[10], (TOKENS2, TOPK), jnp.float32) ** steps_of(arg_keys[10], (TOKENS2, TOPK), ((0, 8),), -0.2, 0.2), 0.25, 1.0)
    expert_gate = noise(arg_keys[11], (EXPERTS, D, FF), D ** -0.5, 0.125, ((0, 8), (2, 4)))
    expert_up = noise(arg_keys[12], (EXPERTS, D, FF), D ** -0.5, 0.125, ((0, 8), (2, 4)))
    expert_down = noise(arg_keys[13], (EXPERTS, FF, D), FF ** -0.5, 0.125, ((0, 8), (1, 4)))
    return dict(mixer_rows=mixer_rows, mixer_gain=mixer_gain, inner_weight=inner_weight, gate_in_weight=gate_in_weight, gate_out_weight=gate_out_weight, conv_taps=conv_taps, mixer_out_weight=mixer_out_weight, routed_rows=routed_rows, routed_gain=routed_gain, route_ids=route_ids, route_weights=route_weights, expert_gate=expert_gate, expert_up=expert_up, expert_down=expert_down)


def rms_scale(row_block, gain_row):
    values = row_block.astype(jnp.float32)
    scaled = values * lax.rsqrt(lax.optimization_barrier(jnp.mean(values * values, axis=-1, keepdims=True)) + 1e-06)
    return (scaled * gain_row).astype(jnp.bfloat16)

def rounded_again(partial_value):
    return lax.optimization_barrier(partial_value.astype(jnp.bfloat16)).astype(jnp.float32)

def reference(mixer_rows, mixer_gain, inner_weight, gate_in_weight, gate_out_weight, conv_taps, mixer_out_weight, routed_rows, routed_gain, route_ids, route_weights, expert_gate, expert_up, expert_down):
    normed = rms_scale(mixer_rows, mixer_gain)
    inner_proj = jnp.dot(normed, inner_weight, preferred_element_type=jnp.float32)
    gate_in = jnp.dot(normed, gate_in_weight, preferred_element_type=jnp.float32)
    conv_input = (gate_in * inner_proj).astype(jnp.bfloat16)
    gate_out = jnp.dot(normed, gate_out_weight, preferred_element_type=jnp.float32)
    padded = jnp.concatenate([jnp.zeros((TAPS - 1, CONV), jnp.bfloat16), conv_input], axis=0).astype(jnp.float32)
    conv_out = jnp.zeros((TOKENS1, CONV), jnp.float32)
    for tap_index in range(TAPS):
        conv_out = conv_out + conv_taps[tap_index] * padded[tap_index:tap_index + TOKENS1]
    gated_conv = (gate_out * conv_out).astype(jnp.bfloat16)
    group_width = CONV // N_TP
    running = jnp.zeros((TOKENS1, D), jnp.float32)
    for piece_index in range(N_TP):
        lower_edge = piece_index * group_width
        partial_value = jnp.dot(gated_conv[:, lower_edge:lower_edge + group_width], mixer_out_weight[lower_edge:lower_edge + group_width], preferred_element_type=jnp.float32)
        running = running + rounded_again(partial_value)
    mixer_output = running.astype(jnp.bfloat16)
    routed_normed = rms_scale(routed_rows, routed_gain)
    blocks = TOKENS2 // TOK2
    flat_ids = route_ids.reshape(blocks, TOK2 * TOPK).astype(jnp.int32)
    onehot = (flat_ids[:, :, None] == jnp.arange(EXPERTS, dtype=jnp.int32)[None, None, :]).astype(jnp.int32)
    earlier = (jnp.cumsum(onehot, axis=1) - onehot).astype(jnp.int32)
    slot_rank = lax.optimization_barrier(jnp.sum(earlier * onehot, axis=2)).astype(jnp.int32)
    block_grid = jnp.broadcast_to(jnp.arange(blocks, dtype=jnp.int32)[:, None], flat_ids.shape)
    token_index = (block_grid * TOK2 + jnp.arange(TOK2 * TOPK, dtype=jnp.int32)[None, :] // TOPK).astype(jnp.int32)
    token_table = jnp.full((EXPERTS, blocks, CAP), TOKENS2, jnp.int32).at[flat_ids, block_grid, slot_rank].set(token_index)
    padded_rows = jnp.concatenate([routed_normed, jnp.zeros((1, D), jnp.bfloat16)], axis=0)
    hidden_width = FF // N_TP

    def one_expert(operands):
        table_rows, gate_w, up_w, down_w = operands
        slot_rows = padded_rows[table_rows.reshape(-1)]
        gate_act = jnp.dot(slot_rows, gate_w, preferred_element_type=jnp.float32)
        up_act = jnp.dot(slot_rows, up_w, preferred_element_type=jnp.float32)
        hidden = (jax.nn.silu(gate_act) * up_act).astype(jnp.bfloat16)
        summed = jnp.zeros((slot_rows.shape[0], D), jnp.float32)
        for piece_index in range(N_TP):
            lower_edge = piece_index * hidden_width
            partial_value = jnp.dot(hidden[:, lower_edge:lower_edge + hidden_width], down_w[lower_edge:lower_edge + hidden_width], preferred_element_type=jnp.float32)
            summed = summed + rounded_again(partial_value)
        return summed.astype(jnp.bfloat16)
    results = lax.map(one_expert, (token_table, expert_gate, expert_up, expert_down))
    results = results.reshape(EXPERTS, blocks, CAP, D)
    picked = results[flat_ids, block_grid, slot_rank].reshape(TOKENS2, TOPK, D).astype(jnp.float32)
    picked = picked * route_weights[:, :, None]
    owner_piece = (slot_rank // (CAP // N_TP)).reshape(TOKENS2, TOPK)
    running_two = jnp.zeros((TOKENS2, D), jnp.float32)
    for piece_index in range(N_TP):
        partial_value = lax.optimization_barrier(jnp.sum(jnp.where((owner_piece == piece_index)[:, :, None], picked, jnp.float32(0.0)), axis=1))
        running_two = running_two + rounded_again(partial_value)
    routed_output = running_two.astype(jnp.bfloat16)
    return (mixer_output, routed_output)
```

```python
import jax
import jax.numpy as jnp
from jax import lax
from jax.experimental import pallas as pl
from jax.experimental.pallas import tpu as pltpu
from jax.sharding import PartitionSpec as P

F32, BF16, I32 = jnp.float32, jnp.bfloat16, jnp.int32
CORES = 2


def rms(values):
    return lax.rsqrt(jnp.mean(values * values, axis=-1, keepdims=True) + 1e-06)


def dot(a, b):
    return jnp.dot(a, b, preferred_element_type=F32)


def make_kernel(experts, groups, tok, picks, width, cap, steps, per, mrows, taps_n, chan):
    high = groups // CORES
    slab = width // groups
    rows = per * cap

    def kernel(
        mixer_rows, mixer_gain, inner_h, gate_in_h, gate_out_h, taps, mixer_out_h,
        routed_rows, routed_gain, ids, weights, gate_h, up_h, down_h,
        out_m, out_r,
        w_inner, w_gin, w_gout, w_mout, w_gate, w_up, w_down,
        disp, slots, part, r1, s2, r2, t3, ret,
        rim, rim_in, m_part, m_r1, m_s2, m_r2,
        w_sem, own_sem,
        d1_s, d1_r, y_s, y_r, b_s, b_r, e_s, e_r, g_s, g_r, ret_s, ret_r,
        rim_s, rim_r, ay_s, ay_r, ab_s, ab_r,
    ):
        me = lax.axis_index("ep")
        t = lax.axis_index("tp")
        yy, cc = t // CORES, t % CORES
        mate = yy * CORES + (1 - cc)
        my_chunk, my_j = me // per, me % per
        sent = []

        def send(src, dst, ssem, rsem, where):
            copy = pltpu.make_async_remote_copy(
                src_ref=src, dst_ref=dst, send_sem=ssem, recv_sem=rsem,
                device_id=where, device_id_type=pl.DeviceIdType.MESH,
            )
            copy.start()
            sent.append(copy)

        def arrive(dst, ssem, rsem):
            pltpu.make_async_remote_copy(
                src_ref=dst, dst_ref=dst, send_sem=ssem, recv_sem=rsem,
                device_id={"tp": mate}, device_id_type=pl.DeviceIdType.MESH,
            ).wait_recv()

        def up_to(dy):
            return lax.rem(yy + dy, high)

        def down_to(dy):
            return lax.rem(yy + high - dy, high)

        loads = []
        for place, (src, dst) in enumerate(
            (
                (inner_h, w_inner), (gate_in_h, w_gin), (gate_out_h, w_gout), (mixer_out_h, w_mout),
                (gate_h, w_gate), (up_h, w_up), (down_h, w_down),
            )
        ):
            copy = pltpu.make_async_copy(src, dst, w_sem.at[place])
            copy.start()
            loads.append(copy)

        barrier = pltpu.get_barrier_semaphore()
        for d in range(1, experts):
            pl.semaphore_signal(
                barrier, inc=1, device_id={"ep": lax.rem(me + d, experts)},
                device_id_type=pl.DeviceIdType.MESH,
            )
        for dy in range(1, high):
            pl.semaphore_signal(
                barrier, inc=1, device_id={"tp": up_to(dy) * CORES + cc},
                device_id_type=pl.DeviceIdType.MESH,
            )
        pl.semaphore_signal(
            barrier, inc=1, device_id={"tp": mate}, device_id_type=pl.DeviceIdType.MESH
        )

        lane = lax.broadcasted_iota(I32, (tok, 128), 1)
        hits = [lane == ids[:, k : k + 1] for k in range(picks)]
        named = sum(h.astype(F32) for h in hits)
        before = (
            lax.broadcasted_iota(I32, (tok, tok), 0) > lax.broadcasted_iota(I32, (tok, tok), 1)
        ).astype(F32).astype(BF16)
        earlier = dot(before, named.astype(BF16))
        slot_lane = lax.broadcasted_iota(I32, (tok, experts * cap), 1)
        pick_map = jnp.zeros((tok, experts * cap), F32)
        sum_map = jnp.zeros((tok, experts * cap), F32)
        for k in range(picks):
            rank = jnp.sum(jnp.where(hits[k], earlier, 0.0), axis=1, keepdims=True).astype(I32)
            at = slot_lane == (ids[:, k : k + 1] * cap + rank)
            pick_map = pick_map + jnp.where(at, 1.0, 0.0)
            sum_map = sum_map + jnp.where(at, weights[:, k : k + 1], 0.0)
        pick_map, sum_map = pick_map.astype(BF16), sum_map.astype(BF16)

        my_cols = pl.ds(pl.multiple_of(t * slab, slab), slab)
        scale = rms(routed_rows[...].astype(F32))
        normed = ((routed_rows[:, my_cols].astype(F32) * scale) * routed_gain[:, my_cols]).astype(BF16)
        disp[...] = (
            lax.dot_general(pick_map, normed, (((0,), (0,)), ((), ())), preferred_element_type=F32)
            .astype(BF16)
            .reshape(experts, cap, slab)
        )
        pl.semaphore_wait(barrier, experts - 1 + high - 1 + 1)

        for i in range(steps):
            chunk = lax.rem(my_chunk + steps - i, steps)
            for j in range(per if i else per - 1):
                jj = j if i else lax.rem(my_j + j + 1, per)
                dest = chunk * per + jj
                send(
                    disp.at[dest], slots.at[t, i, my_j], d1_s.at[i, jj], d1_r.at[i, my_j], {"ep": dest}
                )
        own = pltpu.make_async_copy(disp.at[me], slots.at[t, 0, my_j], own_sem.at[0])
        own.start()

        def stage_a(i):
            for j in range(per if i else per - 1):
                jj = j if i else lax.rem(my_j + j + 1, per)
                arrive(slots.at[t, i, jj], d1_s.at[i, jj], d1_r.at[i, jj])
            if i == 0:
                own.wait()
            for dy in range(1, high):
                send(
                    slots.at[t, i], slots.at[t, i], y_s.at[i, dy - 1], y_r.at[i, dy - 1],
                    {"tp": up_to(dy) * CORES + cc},
                )
            send(slots.at[t, i], slots.at[t, i], b_s.at[i, 0], b_r.at[i, 0], {"tp": mate})

        def stage_b(i):
            for dy in range(1, high):
                block = slots.at[down_to(dy) * CORES + cc, i]
                arrive(block, y_s.at[i, dy - 1], y_r.at[i, dy - 1])
                send(block, block, b_s.at[i, dy], b_r.at[i, dy], {"tp": mate})

        def stage_c(i):
            for dy in range(high):
                arrive(
                    slots.at[down_to(dy) * CORES + (1 - cc), i], b_s.at[i, dy], b_r.at[i, dy]
                )
            if i == 0:
                for copy in loads[4:]:
                    copy.wait()
            x = jnp.concatenate([slots[q, i].reshape(rows, slab) for q in range(groups)], axis=1)
            gate, up = dot(x, w_gate[...]), dot(x, w_up[...])
            hidden = (gate / (1.0 + jnp.exp(-gate)) * up).astype(BF16)
            for q in range(groups):
                part[i, q % CORES, q // CORES] = dot(
                    hidden, w_down[:, q * slab : (q + 1) * slab]
                ).astype(BF16)
            send(part.at[i, 1 - cc], r1.at[i], e_s.at[i], e_r.at[i], {"tp": mate})

        def pair_sum(i, part_i, r1_i, s2_i, r2_i):
            arrive(r1_i, e_s.at[i], e_r.at[i])
            for y in range(high):
                s2_i[y] = (part_i[cc, y].astype(F32) + r1_i[y].astype(F32)).astype(BF16)
            for dy in range(1, high):
                send(
                    s2_i.at[up_to(dy)], r2_i.at[dy - 1], g_s.at[i, dy - 1], g_r.at[i, dy - 1],
                    {"tp": up_to(dy) * CORES + cc},
                )

        def chip_sum(i, s2_i, r2_i):
            total = s2_i[yy].astype(F32)
            for dy in range(1, high):
                arrive(r2_i.at[dy - 1], g_s.at[i, dy - 1], g_r.at[i, dy - 1])
                total = total + r2_i[dy - 1].astype(F32)
            return total.astype(BF16)

        def stage_e(i):
            pair_sum(i, part.at[i], r1.at[i], s2.at[i], r2.at[i])

        def stage_g(i):
            t3[i] = chip_sum(i, s2.at[i], r2.at[i]).reshape(per, cap, slab)
            chunk = lax.rem(my_chunk + i, steps)
            for j in range(per if i else per - 1):
                jj = j if i else lax.rem(my_j + j + 1, per)
                dest = chunk * per + jj
                send(t3.at[i, jj], ret.at[me], ret_s.at[i, jj], ret_r.at[me], {"ep": dest})
            if i == 0:
                ret[me] = t3[0, my_j]

        def spread(which, out, value):
            out[:, my_cols] = value
            window = out.at[:, my_cols]
            for dy in range(1, high):
                send(
                    window, window, ay_s.at[which, dy - 1], ay_r.at[which, dy - 1],
                    {"tp": up_to(dy) * CORES + cc},
                )
            send(window, window, ab_s.at[which, 0], ab_r.at[which, 0], {"tp": mate})

        def window_of(out, group):
            return out.at[:, pl.ds(pl.multiple_of(group * slab, slab), slab)]

        def spread_on(which, out):
            for dy in range(1, high):
                window = window_of(out, down_to(dy) * CORES + cc)
                arrive(window, ay_s.at[which, dy - 1], ay_r.at[which, dy - 1])
                send(window, window, ab_s.at[which, dy], ab_r.at[which, dy], {"tp": mate})

        def spread_end(which, out):
            for dy in range(high):
                arrive(
                    window_of(out, down_to(dy) * CORES + (1 - cc)),
                    ab_s.at[which, dy], ab_r.at[which, dy],
                )

        for copy in loads[:4]:
            copy.wait()
        mixed = mixer_rows[...].astype(F32)
        mixed = ((mixed * rms(mixed)) * mixer_gain[...]).astype(BF16)
        conv_input = (dot(mixed, w_gin[...]) * dot(mixed, w_inner[...])).astype(BF16)
        edge = rim.shape[0]
        rim[...] = conv_input[mrows - edge :]
        send(rim, rim_in, rim_s.at[0], rim_r.at[0], {"ep": lax.rem(me + 1, experts)})
        gate_out = dot(mixed, w_gout[...])
        stage_a(0)
        arrive(rim_in, rim_s.at[0], rim_r.at[0])
        first = jnp.where(me == 0, 0.0, rim_in[...].astype(F32))
        extended = jnp.concatenate([first, conv_input.astype(F32)], axis=0)
        conv = jnp.zeros((mrows, chan), F32)
        for k in range(taps_n):
            start = edge - (taps_n - 1) + k
            conv = conv + taps[k : k + 1, :] * extended[start : start + mrows]
        gated = (gate_out * conv).astype(BF16)
        for q in range(groups):
            m_part[q % CORES, q // CORES] = dot(gated, w_mout[:, q * slab : (q + 1) * slab]).astype(BF16)
        send(m_part.at[1 - cc], m_r1, e_s.at[steps], e_r.at[steps], {"tp": mate})

        for s in range(1, steps + 4):
            if s < steps:
                stage_a(s)
            if s - 1 < steps:
                stage_b(s - 1)
            if s == 1:
                pair_sum(steps, m_part, m_r1, m_s2, m_r2)
            if 0 <= s - 2 < steps:
                stage_e(s - 2)
            if s == 2:
                spread(0, out_m, chip_sum(steps, m_s2, m_r2))
            if s == 3:
                spread_on(0, out_m)
            if s - 1 < steps:
                stage_c(s - 1)
            if 0 <= s - 3 < steps:
                stage_g(s - 3)

        for d in range(1, experts):
            e = lax.rem(me + d, experts)
            arrive(ret.at[e], ret_s.at[0, 0], ret_r.at[e])
        spread(1, out_r, dot(sum_map, ret[...].reshape(experts * cap, slab)).astype(BF16))
        spread_on(1, out_r)
        spread_end(0, out_m)
        spread_end(1, out_r)
        for copy in sent:
            copy.wait_send()

    edge = 16 * -(-(taps_n - 1) // 16)
    dma = pltpu.SemaphoreType.DMA
    far = max(1, high - 1)
    hid_scratch = lambda shape, kind=BF16: pltpu.VMEM(shape, kind)
    v = hid_scratch

    def scratch(hid):
        return [
            v((width, chan)), v((width, chan)), v((width, chan)), v((chan, width)),
            v((width, hid)), v((width, hid)), v((hid, width)),
            v((experts, cap, slab)), v((groups, steps, per, cap, slab)),
            v((steps, CORES, high, rows, slab)), v((steps, high, rows, slab)),
            v((steps, high, rows, slab)), v((steps, far, rows, slab)),
            v((steps, per, cap, slab)), v((experts, cap, slab)),
            v((edge, chan)), v((edge, chan)),
            v((CORES, high, mrows, slab)), v((high, mrows, slab)), v((high, mrows, slab)),
            v((far, mrows, slab)),
            dma((7,)), dma((1,)),
            dma((steps, per)), dma((steps, per)), dma((steps, far)), dma((steps, far)),
            dma((steps, high)), dma((steps, high)), dma((steps + 1,)), dma((steps + 1,)),
            dma((steps + 1, far)), dma((steps + 1, far)), dma((steps, per)), dma((experts,)),
            dma((1,)), dma((1,)), dma((2, far)), dma((2, far)), dma((2, high)), dma((2, high)),
        ]

    return kernel, scratch


def on_device(
    mixer_rows, mixer_gain, inner_weight, gate_in_weight, gate_out_weight, conv_taps,
    mixer_out_weight, routed_rows, routed_gain, route_ids, route_weights,
    expert_gate, expert_up, expert_down,
):
    experts, groups = lax.axis_size("ep"), lax.axis_size("tp")
    tok, picks = route_ids.shape
    width = routed_rows.shape[1]
    cap = 2 * tok * picks // experts
    per = max(1, min(experts, tok // cap))
    steps = experts // per
    mrows = mixer_rows.shape[0]
    taps_n, chan = conv_taps.shape
    kernel, scratch = make_kernel(
        experts, groups, tok, picks, width, cap, steps, per, mrows, taps_n, chan
    )
    near, far = pl.BlockSpec(memory_space=pltpu.VMEM), pl.BlockSpec(memory_space=pl.ANY)
    return pl.pallas_call(
        kernel,
        out_shape=(
            jax.ShapeDtypeStruct(mixer_rows.shape, BF16),
            jax.ShapeDtypeStruct(routed_rows.shape, BF16),
        ),
        in_specs=[near, near, far, far, far, near, far, near, near, near, near, far, far, far],
        out_specs=(near, near),
        scratch_shapes=scratch(expert_gate.shape[2]),
        compiler_params=pltpu.CompilerParams(
            collective_id=0, has_side_effects=True, vmem_limit_bytes=60 * 1024 * 1024
        ),
        name="mixer_and_experts",
    )(
        mixer_rows, mixer_gain[None, :], inner_weight, gate_in_weight, gate_out_weight, conv_taps,
        mixer_out_weight, routed_rows, routed_gain[None, :], route_ids, route_weights,
        expert_gate[0], expert_up[0], expert_down[0],
    )


def solution(mesh):
    return jax.shard_map(
        on_device,
        mesh=mesh,
        in_specs=(
            P("ep", None), P(), P(None, "tp"), P(None, "tp"), P(None, "tp"), P(None, "tp"),
            P("tp", None), P("ep", None), P(), P("ep", None), P("ep", None),
            P("ep", None, "tp"), P("ep", None, "tp"), P("ep", "tp", None),
        ),
        out_specs=(P("ep", None), P("ep", None)),
        check_vma=False,
    )
```

```python
import jax
import jax.numpy as jnp
from jax import lax
from jax.experimental import pallas as pl
from jax.experimental.pallas import tpu as pltpu
from jax.sharding import PartitionSpec as P

F32, BF16, I32 = jnp.float32, jnp.bfloat16, jnp.int32
CORES = 2


def rms(values):
    return lax.rsqrt(jnp.mean(values * values, axis=-1, keepdims=True) + 1e-06)


def dot(a, b):
    return jnp.dot(a, b, preferred_element_type=F32)


def make_kernel(experts, groups, tok, picks, width, cap, steps, per, mrows, taps_n, chan):
    high = groups // CORES
    whole = min(2, steps)
    slab = width // groups
    rows = per * cap

    def kernel(
        mixer_rows, mixer_gain, inner_h, gate_in_h, gate_out_h, taps, mixer_out_h,
        routed_rows, routed_gain, ids, weights, gate_h, up_h, down_h,
        out_m, out_r,
        w_inner, w_gin, w_gout, w_mout, w_gate, w_up, w_down,
        disp, slots, part, r1, s2, r2, t3, ret,
        rim, rim_in, m_part, m_r1, m_s2, m_r2,
        w_sem, own_sem,
        d1_s, d1_r, y_s, y_r, b_s, b_r, e_s, e_r, g_s, g_r, ret_s, ret_r,
        rim_s, rim_r, ay_s, ay_r, ab_s, ab_r,
    ):
        me = lax.axis_index("ep")
        t = lax.axis_index("tp")
        yy, cc = t // CORES, t % CORES
        mate = yy * CORES + (1 - cc)
        my_chunk, my_j = me // per, me % per
        sent = []

        def send(src, dst, ssem, rsem, where):
            copy = pltpu.make_async_remote_copy(
                src_ref=src, dst_ref=dst, send_sem=ssem, recv_sem=rsem,
                device_id=where, device_id_type=pl.DeviceIdType.MESH,
            )
            copy.start()
            sent.append(copy)

        def arrive(dst, ssem, rsem):
            pltpu.make_async_remote_copy(
                src_ref=dst, dst_ref=dst, send_sem=ssem, recv_sem=rsem,
                device_id={"tp": mate}, device_id_type=pl.DeviceIdType.MESH,
            ).wait_recv()

        def up_to(dy):
            return lax.rem(yy + dy, high)

        def down_to(dy):
            return lax.rem(yy + high - dy, high)

        loads = []
        for place, (src, dst) in enumerate(
            (
                (inner_h, w_inner), (gate_in_h, w_gin), (gate_out_h, w_gout), (mixer_out_h, w_mout),
                (gate_h, w_gate), (up_h, w_up), (down_h, w_down),
            )
        ):
            copy = pltpu.make_async_copy(src, dst, w_sem.at[place])
            copy.start()
            loads.append(copy)

        barrier = pltpu.get_barrier_semaphore()
        for d in range(1, experts):
            pl.semaphore_signal(
                barrier, inc=1, device_id={"ep": lax.rem(me + d, experts)},
                device_id_type=pl.DeviceIdType.MESH,
            )
        for dy in range(1, high):
            pl.semaphore_signal(
                barrier, inc=1, device_id={"tp": up_to(dy) * CORES + cc},
                device_id_type=pl.DeviceIdType.MESH,
            )
        pl.semaphore_signal(
            barrier, inc=1, device_id={"tp": mate}, device_id_type=pl.DeviceIdType.MESH
        )

        row = lax.broadcasted_iota(I32, (128, tok), 0)
        hits = [row == ids[k : k + 1, :] for k in range(picks)]
        named = sum(h.astype(F32) for h in hits)
        before = (
            lax.broadcasted_iota(I32, (tok, tok), 0) < lax.broadcasted_iota(I32, (tok, tok), 1)
        ).astype(F32).astype(BF16)
        earlier = dot(named.astype(BF16), before)
        slot_row = lax.broadcasted_iota(I32, (experts * cap, tok), 0)
        pick_map = jnp.zeros((experts * cap, tok), F32)
        sum_map = jnp.zeros((experts * cap, tok), F32)
        for k in range(picks):
            rank = jnp.sum(jnp.where(hits[k], earlier, 0.0), axis=0, keepdims=True).astype(I32)
            at = slot_row == (ids[k : k + 1, :] * cap + rank)
            pick_map = pick_map + jnp.where(at, 1.0, 0.0)
            sum_map = sum_map + jnp.where(at, weights[k : k + 1, :], 0.0)
        pick_map, sum_map = pick_map.astype(BF16), sum_map.astype(BF16)

        my_cols = pl.ds(pl.multiple_of(t * slab, slab), slab)
        scale = rms(routed_rows[...].astype(F32))
        for y in range(high):
            cols = pl.ds(pl.multiple_of((y * CORES + cc) * slab, slab), slab)
            normed = ((routed_rows[:, cols].astype(F32) * scale) * routed_gain[:, cols]).astype(BF16)
            disp[y] = dot(pick_map, normed).astype(BF16).reshape(experts, cap, slab)
        pl.semaphore_wait(barrier, experts - 1 + high - 1 + 1)

        def others(i):
            return [j if i else lax.rem(my_j + j + 1, per) for j in range(per if i else per - 1)]

        def partner(i):
            chunk = my_chunk
            for bit in (1 << n for n in range(i.bit_length())):
                if i & bit:
                    chunk = chunk + bit - 2 * bit * lax.rem(chunk // bit, 2)
            return chunk

        def slabs(i):
            return range(high if i < whole else 1)

        for i in range(steps):
            for jj in others(i):
                dest = partner(i) * per + jj
                for dy in slabs(i):
                    y = down_to(dy)
                    send(
                        disp.at[y, dest], slots.at[y * CORES + cc, i, my_j],
                        d1_s.at[i, jj, dy], d1_r.at[i, my_j, dy], {"ep": dest},
                    )
        own = []
        for y in range(high):
            copy = pltpu.make_async_copy(
                disp.at[y, me], slots.at[y * CORES + cc, 0, my_j], own_sem.at[y]
            )
            copy.start()
            own.append(copy)

        def stage_a(i):
            for jj in others(i):
                for dy in slabs(i):
                    arrive(
                        slots.at[down_to(dy) * CORES + cc, i, jj], d1_s.at[i, jj, dy], d1_r.at[i, jj, dy]
                    )
            if i == 0:
                for copy in own:
                    copy.wait()
            if i >= whole:
                for dy in range(1, high):
                    send(
                        slots.at[t, i], slots.at[t, i], y_s.at[i, dy - 1], y_r.at[i, dy - 1],
                        {"tp": up_to(dy) * CORES + cc},
                    )
            for dy in slabs(i):
                block = slots.at[down_to(dy) * CORES + cc, i]
                send(block, block, b_s.at[i, dy], b_r.at[i, dy], {"tp": mate})

        def stage_b(i):
            if i < whole:
                return
            for dy in range(1, high):
                block = slots.at[down_to(dy) * CORES + cc, i]
                arrive(block, y_s.at[i, dy - 1], y_r.at[i, dy - 1])
                send(block, block, b_s.at[i, dy], b_r.at[i, dy], {"tp": mate})

        def stage_c(i):
            for dy in range(high):
                arrive(
                    slots.at[down_to(dy) * CORES + (1 - cc), i], b_s.at[i, dy], b_r.at[i, dy]
                )
            if i == 0:
                for copy in loads[4:]:
                    copy.wait()
            x = jnp.concatenate([slots[q, i].reshape(rows, slab) for q in range(groups)], axis=1)
            gate, up = dot(x, w_gate[...]), dot(x, w_up[...])
            hidden = (gate / (1.0 + jnp.exp(-gate)) * up).astype(BF16)
            for q in range(groups):
                part[i, q % CORES, q // CORES] = dot(
                    hidden, w_down[:, q * slab : (q + 1) * slab]
                ).astype(BF16)
            send(part.at[i, 1 - cc], r1.at[i], e_s.at[i], e_r.at[i], {"tp": mate})

        def pair_sum(i, part_i, r1_i, s2_i, r2_i):
            arrive(r1_i, e_s.at[i], e_r.at[i])
            for y in range(high):
                s2_i[y] = (part_i[cc, y].astype(F32) + r1_i[y].astype(F32)).astype(BF16)
            for dy in range(1, high):
                send(
                    s2_i.at[up_to(dy)], r2_i.at[dy - 1], g_s.at[i, dy - 1], g_r.at[i, dy - 1],
                    {"tp": up_to(dy) * CORES + cc},
                )

        def chip_sum(i, s2_i, r2_i):
            total = s2_i[yy].astype(F32)
            for dy in range(1, high):
                arrive(r2_i.at[dy - 1], g_s.at[i, dy - 1], g_r.at[i, dy - 1])
                total = total + r2_i[dy - 1].astype(F32)
            return total.astype(BF16)

        def stage_e(i):
            pair_sum(i, part.at[i], r1.at[i], s2.at[i], r2.at[i])

        def stage_g(i):
            t3[i] = chip_sum(i, s2.at[i], r2.at[i]).reshape(per, cap, slab)
            for jj in others(i):
                dest = partner(i) * per + jj
                send(t3.at[i, jj], ret.at[me], ret_s.at[i, jj], ret_r.at[me], {"ep": dest})
            if i == 0:
                ret[me] = t3[0, my_j]

        def spread(which, out, value):
            out[:, my_cols] = value
            window = out.at[:, my_cols]
            for dy in range(1, high):
                send(
                    window, window, ay_s.at[which, dy - 1], ay_r.at[which, dy - 1],
                    {"tp": up_to(dy) * CORES + cc},
                )
            send(window, window, ab_s.at[which, 0], ab_r.at[which, 0], {"tp": mate})

        def window_of(out, group):
            return out.at[:, pl.ds(pl.multiple_of(group * slab, slab), slab)]

        def spread_on(which, out):
            for dy in range(1, high):
                window = window_of(out, down_to(dy) * CORES + cc)
                arrive(window, ay_s.at[which, dy - 1], ay_r.at[which, dy - 1])
                send(window, window, ab_s.at[which, dy], ab_r.at[which, dy], {"tp": mate})

        def spread_end(which, out):
            for dy in range(high):
                arrive(
                    window_of(out, down_to(dy) * CORES + (1 - cc)),
                    ab_s.at[which, dy], ab_r.at[which, dy],
                )

        for copy in loads[:4]:
            copy.wait()
        mixed = mixer_rows[...].astype(F32)
        mixed = ((mixed * rms(mixed)) * mixer_gain[...]).astype(BF16)
        conv_input = (dot(mixed, w_gin[...]) * dot(mixed, w_inner[...])).astype(BF16)
        edge = rim.shape[0]
        rim[...] = conv_input[mrows - edge :]
        send(rim, rim_in, rim_s.at[0], rim_r.at[0], {"ep": lax.rem(me + 1, experts)})
        gate_out = dot(mixed, w_gout[...])
        stage_a(0)
        arrive(rim_in, rim_s.at[0], rim_r.at[0])
        first = jnp.where(me == 0, 0.0, rim_in[...].astype(F32))
        extended = jnp.concatenate([first, conv_input.astype(F32)], axis=0)
        conv = jnp.zeros((mrows, chan), F32)
        for k in range(taps_n):
            start = edge - (taps_n - 1) + k
            conv = conv + taps[k : k + 1, :] * extended[start : start + mrows]
        gated = (gate_out * conv).astype(BF16)
        for q in range(groups):
            m_part[q % CORES, q // CORES] = dot(gated, w_mout[:, q * slab : (q + 1) * slab]).astype(BF16)
        send(m_part.at[1 - cc], m_r1, e_s.at[steps], e_r.at[steps], {"tp": mate})

        for s in range(steps):
            stage_b(s)
            stage_c(s)
            if s + 1 < steps:
                stage_a(s + 1)
            if s == 0:
                pair_sum(steps, m_part, m_r1, m_s2, m_r2)
            stage_e(s)
            if s == 1:
                spread(0, out_m, chip_sum(steps, m_s2, m_r2))
            if s == 2:
                spread_on(0, out_m)
            if s >= 1:
                stage_g(s - 1)
        stage_g(steps - 1)

        for d in range(1, experts):
            e = lax.rem(me + d, experts)
            arrive(ret.at[e], ret_s.at[0, 0], ret_r.at[e])
        summed = lax.dot_general(
            sum_map, ret[...].reshape(experts * cap, slab), (((0,), (0,)), ((), ())),
            preferred_element_type=F32,
        )
        spread(1, out_r, summed.astype(BF16))
        spread_on(1, out_r)
        spread_end(0, out_m)
        spread_end(1, out_r)
        for copy in sent:
            copy.wait_send()

    edge = 16 * -(-(taps_n - 1) // 16)
    dma = pltpu.SemaphoreType.DMA
    far = max(1, high - 1)
    hid_scratch = lambda shape, kind=BF16: pltpu.VMEM(shape, kind)
    v = hid_scratch

    def scratch(hid):
        return [
            v((width, chan)), v((width, chan)), v((width, chan)), v((chan, width)),
            v((width, hid)), v((width, hid)), v((hid, width)),
            v((high, experts, cap, slab)), v((groups, steps, per, cap, slab)),
            v((steps, CORES, high, rows, slab)), v((steps, high, rows, slab)),
            v((steps, high, rows, slab)), v((steps, far, rows, slab)),
            v((steps, per, cap, slab)), v((experts, cap, slab)),
            v((edge, chan)), v((edge, chan)),
            v((CORES, high, mrows, slab)), v((high, mrows, slab)), v((high, mrows, slab)),
            v((far, mrows, slab)),
            dma((7,)), dma((high,)),
            dma((steps, per, high)), dma((steps, per, high)), dma((steps, far)), dma((steps, far)),
            dma((steps, high)), dma((steps, high)), dma((steps + 1,)), dma((steps + 1,)),
            dma((steps + 1, far)), dma((steps + 1, far)), dma((steps, per)), dma((experts,)),
            dma((1,)), dma((1,)), dma((2, far)), dma((2, far)), dma((2, high)), dma((2, high)),
        ]

    return kernel, scratch


def on_device(
    mixer_rows, mixer_gain, inner_weight, gate_in_weight, gate_out_weight, conv_taps,
    mixer_out_weight, routed_rows, routed_gain, route_ids, route_weights,
    expert_gate, expert_up, expert_down,
):
    experts, groups = lax.axis_size("ep"), lax.axis_size("tp")
    tok, picks = route_ids.shape
    width = routed_rows.shape[1]
    cap = 2 * tok * picks // experts
    per = max(1, min(experts, tok // cap))
    steps = experts // per
    mrows = mixer_rows.shape[0]
    taps_n, chan = conv_taps.shape
    kernel, scratch = make_kernel(
        experts, groups, tok, picks, width, cap, steps, per, mrows, taps_n, chan
    )
    near, far = pl.BlockSpec(memory_space=pltpu.VMEM), pl.BlockSpec(memory_space=pl.ANY)
    return pl.pallas_call(
        kernel,
        out_shape=(
            jax.ShapeDtypeStruct(mixer_rows.shape, BF16),
            jax.ShapeDtypeStruct(routed_rows.shape, BF16),
        ),
        in_specs=[near, near, far, far, far, near, far, near, near, near, near, far, far, far],
        out_specs=(near, near),
        scratch_shapes=scratch(expert_gate.shape[2]),
        compiler_params=pltpu.CompilerParams(
            collective_id=0, has_side_effects=True, vmem_limit_bytes=60 * 1024 * 1024
        ),
        name="mixer_and_experts",
    )(
        mixer_rows, mixer_gain[None, :], inner_weight, gate_in_weight, gate_out_weight, conv_taps,
        mixer_out_weight, routed_rows, routed_gain[None, :], route_ids.T, route_weights.T,
        expert_gate[0], expert_up[0], expert_down[0],
    )


def solution(mesh):
    return jax.shard_map(
        on_device,
        mesh=mesh,
        in_specs=(
            P("ep", None), P(), P(None, "tp"), P(None, "tp"), P(None, "tp"), P(None, "tp"),
            P("tp", None), P("ep", None), P(), P("ep", None), P("ep", None),
            P("ep", None, "tp"), P("ep", None, "tp"), P("ep", "tp", None),
        ),
        out_specs=(P("ep", None), P("ep", None)),
        check_vma=False,
    )
```

```python
import jax
import jax.numpy as jnp
from jax import lax
from jax.experimental import pallas as pl
from jax.experimental.pallas import tpu as pltpu
from jax.sharding import PartitionSpec as P

F32, BF16, I32 = jnp.float32, jnp.bfloat16, jnp.int32
CORES = 2


def rms(values):
    return lax.rsqrt(jnp.mean(values * values, axis=-1, keepdims=True) + 1e-06)


def dot(a, b):
    return jnp.dot(a, b, preferred_element_type=F32)


def make_kernel(experts, groups, tok, picks, width, cap, steps, per, mrows, taps_n, chan):
    high = groups // CORES
    whole = 1
    half = steps // 2
    order = list(range(half, steps)) + list(range(half - 1, -1, -1))
    slab = width // groups
    rows = per * cap

    def kernel(
        mixer_rows, mixer_gain, inner_h, gate_in_h, gate_out_h, taps, mixer_out_h,
        routed_rows, routed_gain, ids, weights, gate_h, up_h, down_h,
        out_m, out_r,
        w_inner, w_gin, w_gout, w_mout, w_gate, w_up, w_down,
        disp, slots, part, r1, s2, r2, t3, ret,
        rim, rim_in, m_part, m_r1, m_s2, m_r2,
        w_sem, own_sem,
        d1_s, d1_r, y_s, y_r, b_s, b_r, e_s, e_r, g_s, g_r, ret_s, ret_r,
        rim_s, rim_r, ay_s, ay_r, ab_s, ab_r,
    ):
        me = lax.axis_index("ep")
        t = lax.axis_index("tp")
        yy, cc = t // CORES, t % CORES
        mate = yy * CORES + (1 - cc)
        my_chunk, my_j = me // per, me % per
        sent = []

        def send(src, dst, ssem, rsem, where):
            copy = pltpu.make_async_remote_copy(
                src_ref=src, dst_ref=dst, send_sem=ssem, recv_sem=rsem,
                device_id=where, device_id_type=pl.DeviceIdType.MESH,
            )
            copy.start()
            sent.append(copy)

        def arrive(dst, ssem, rsem):
            pltpu.make_async_remote_copy(
                src_ref=dst, dst_ref=dst, send_sem=ssem, recv_sem=rsem,
                device_id={"tp": mate}, device_id_type=pl.DeviceIdType.MESH,
            ).wait_recv()

        def up_to(dy):
            return lax.rem(yy + dy, high)

        def down_to(dy):
            return lax.rem(yy + high - dy, high)

        loads = []
        for place, (src, dst) in enumerate(
            (
                (inner_h, w_inner), (gate_in_h, w_gin), (gate_out_h, w_gout), (mixer_out_h, w_mout),
                (gate_h, w_gate), (up_h, w_up), (down_h, w_down),
            )
        ):
            copy = pltpu.make_async_copy(src, dst, w_sem.at[place])
            copy.start()
            loads.append(copy)

        barrier = pltpu.get_barrier_semaphore()
        for d in range(1, experts):
            pl.semaphore_signal(
                barrier, inc=1, device_id={"ep": lax.rem(me + d, experts)},
                device_id_type=pl.DeviceIdType.MESH,
            )
        for dy in range(1, high):
            pl.semaphore_signal(
                barrier, inc=1, device_id={"tp": up_to(dy) * CORES + cc},
                device_id_type=pl.DeviceIdType.MESH,
            )
        pl.semaphore_signal(
            barrier, inc=1, device_id={"tp": mate}, device_id_type=pl.DeviceIdType.MESH
        )

        row = lax.broadcasted_iota(I32, (128, tok), 0)
        hits = [row == ids[k : k + 1, :] for k in range(picks)]
        named = sum(h.astype(F32) for h in hits)
        before = (
            lax.broadcasted_iota(I32, (tok, tok), 0) < lax.broadcasted_iota(I32, (tok, tok), 1)
        ).astype(F32).astype(BF16)
        earlier = dot(named.astype(BF16), before)
        slot_row = lax.broadcasted_iota(I32, (experts * cap, tok), 0)
        pick_map = jnp.zeros((experts * cap, tok), F32)
        sum_map = jnp.zeros((experts * cap, tok), F32)
        for k in range(picks):
            rank = jnp.sum(jnp.where(hits[k], earlier, 0.0), axis=0, keepdims=True).astype(I32)
            at = slot_row == (ids[k : k + 1, :] * cap + rank)
            pick_map = pick_map + jnp.where(at, 1.0, 0.0)
            sum_map = sum_map + jnp.where(at, weights[k : k + 1, :], 0.0)
        pick_map, sum_map = pick_map.astype(BF16), sum_map.astype(BF16)

        my_cols = pl.ds(pl.multiple_of(t * slab, slab), slab)
        scale = rms(routed_rows[...].astype(F32))
        for y in range(high):
            cols = pl.ds(pl.multiple_of((y * CORES + cc) * slab, slab), slab)
            normed = ((routed_rows[:, cols].astype(F32) * scale) * routed_gain[:, cols]).astype(BF16)
            disp[y] = dot(pick_map, normed).astype(BF16).reshape(experts, cap, slab)
        pl.semaphore_wait(barrier, experts - 1 + high - 1 + 1)

        def others(i):
            return [j if i else lax.rem(my_j + j + 1, per) for j in range(per if i else per - 1)]

        def partner(i):
            chunk = my_chunk
            for bit in (1 << n for n in range(i.bit_length())):
                if i & bit:
                    chunk = chunk + bit - 2 * bit * lax.rem(chunk // bit, 2)
            return chunk

        def slabs(i):
            return range(high if i < whole else 1)

        for i in order:
            for jj in others(i):
                dest = partner(i) * per + jj
                for dy in slabs(i):
                    y = down_to(dy)
                    send(
                        disp.at[y, dest], slots.at[y * CORES + cc, i, my_j],
                        d1_s.at[i, jj, dy], d1_r.at[i, my_j, dy], {"ep": dest},
                    )
        own = []
        for y in range(high):
            copy = pltpu.make_async_copy(
                disp.at[y, me], slots.at[y * CORES + cc, 0, my_j], own_sem.at[y]
            )
            copy.start()
            own.append(copy)

        def stage_a(i):
            for jj in others(i):
                for dy in slabs(i):
                    arrive(
                        slots.at[down_to(dy) * CORES + cc, i, jj], d1_s.at[i, jj, dy], d1_r.at[i, jj, dy]
                    )
            if i == 0:
                for copy in own:
                    copy.wait()
            if i >= whole:
                for dy in range(1, high):
                    send(
                        slots.at[t, i], slots.at[t, i], y_s.at[i, dy - 1], y_r.at[i, dy - 1],
                        {"tp": up_to(dy) * CORES + cc},
                    )
            for dy in slabs(i):
                block = slots.at[down_to(dy) * CORES + cc, i]
                send(block, block, b_s.at[i, dy], b_r.at[i, dy], {"tp": mate})

        def stage_b(i):
            if i < whole:
                return
            for dy in range(1, high):
                block = slots.at[down_to(dy) * CORES + cc, i]
                arrive(block, y_s.at[i, dy - 1], y_r.at[i, dy - 1])
                send(block, block, b_s.at[i, dy], b_r.at[i, dy], {"tp": mate})

        def stage_c(i):
            for dy in range(high):
                arrive(
                    slots.at[down_to(dy) * CORES + (1 - cc), i], b_s.at[i, dy], b_r.at[i, dy]
                )
            x = jnp.concatenate([slots[q, i].reshape(rows, slab) for q in range(groups)], axis=1)
            gate, up = dot(x, w_gate[...]), dot(x, w_up[...])
            hidden = (gate / (1.0 + jnp.exp(-gate)) * up).astype(BF16)
            for q in range(groups):
                part[i, q % CORES, q // CORES] = dot(
                    hidden, w_down[:, q * slab : (q + 1) * slab]
                ).astype(BF16)
            send(part.at[i, 1 - cc], r1.at[i], e_s.at[i], e_r.at[i], {"tp": mate})

        def pair_sum(i, part_i, r1_i, s2_i, r2_i):
            arrive(r1_i, e_s.at[i], e_r.at[i])
            for y in range(high):
                s2_i[y] = (part_i[cc, y].astype(F32) + r1_i[y].astype(F32)).astype(BF16)
            for dy in range(1, high):
                send(
                    s2_i.at[up_to(dy)], r2_i.at[dy - 1], g_s.at[i, dy - 1], g_r.at[i, dy - 1],
                    {"tp": up_to(dy) * CORES + cc},
                )

        def chip_sum(i, s2_i, r2_i):
            total = s2_i[yy].astype(F32)
            for dy in range(1, high):
                arrive(r2_i.at[dy - 1], g_s.at[i, dy - 1], g_r.at[i, dy - 1])
                total = total + r2_i[dy - 1].astype(F32)
            return total.astype(BF16)

        def stage_e(i):
            pair_sum(i, part.at[i], r1.at[i], s2.at[i], r2.at[i])

        def stage_g(i):
            t3[i] = chip_sum(i, s2.at[i], r2.at[i]).reshape(per, cap, slab)
            for jj in others(i):
                dest = partner(i) * per + jj
                send(t3.at[i, jj], ret.at[me], ret_s.at[i, jj], ret_r.at[me], {"ep": dest})
            if i == 0:
                ret[me] = t3[0, my_j]

        def spread(which, out, value):
            out[:, my_cols] = value
            window = out.at[:, my_cols]
            for dy in range(1, high):
                send(
                    window, window, ay_s.at[which, dy - 1], ay_r.at[which, dy - 1],
                    {"tp": up_to(dy) * CORES + cc},
                )
            send(window, window, ab_s.at[which, 0], ab_r.at[which, 0], {"tp": mate})

        def window_of(out, group):
            return out.at[:, pl.ds(pl.multiple_of(group * slab, slab), slab)]

        def spread_on(which, out):
            for dy in range(1, high):
                window = window_of(out, down_to(dy) * CORES + cc)
                arrive(window, ay_s.at[which, dy - 1], ay_r.at[which, dy - 1])
                send(window, window, ab_s.at[which, dy], ab_r.at[which, dy], {"tp": mate})

        def spread_end(which, out):
            for dy in range(high):
                arrive(
                    window_of(out, down_to(dy) * CORES + (1 - cc)),
                    ab_s.at[which, dy], ab_r.at[which, dy],
                )

        for copy in loads[:4]:
            copy.wait()
        mixed = mixer_rows[...].astype(F32)
        mixed = ((mixed * rms(mixed)) * mixer_gain[...]).astype(BF16)
        conv_input = (dot(mixed, w_gin[...]) * dot(mixed, w_inner[...])).astype(BF16)
        edge = rim.shape[0]
        rim[...] = conv_input[mrows - edge :]
        send(rim, rim_in, rim_s.at[0], rim_r.at[0], {"ep": lax.rem(me + 1, experts)})
        gate_out = dot(mixed, w_gout[...])
        stage_a(order[0])
        arrive(rim_in, rim_s.at[0], rim_r.at[0])
        first = jnp.where(me == 0, 0.0, rim_in[...].astype(F32))
        extended = jnp.concatenate([first, conv_input.astype(F32)], axis=0)
        conv = jnp.zeros((mrows, chan), F32)
        for k in range(taps_n):
            start = edge - (taps_n - 1) + k
            conv = conv + taps[k : k + 1, :] * extended[start : start + mrows]
        gated = (gate_out * conv).astype(BF16)
        for q in range(groups):
            m_part[q % CORES, q // CORES] = dot(gated, w_mout[:, q * slab : (q + 1) * slab]).astype(BF16)
        send(m_part.at[1 - cc], m_r1, e_s.at[steps], e_r.at[steps], {"tp": mate})

        for copy in loads[4:]:
            copy.wait()
        for s in range(steps):
            stage_b(order[s])
            stage_c(order[s])
            if s + 1 < steps:
                stage_a(order[s + 1])
            if s == 0:
                pair_sum(steps, m_part, m_r1, m_s2, m_r2)
            stage_e(order[s])
            if s == 1:
                spread(0, out_m, chip_sum(steps, m_s2, m_r2))
            if s == 2:
                spread_on(0, out_m)
            if s >= 1:
                stage_g(order[s - 1])
        stage_g(order[steps - 1])

        for d in range(1, experts):
            e = lax.rem(me + d, experts)
            arrive(ret.at[e], ret_s.at[0, 0], ret_r.at[e])
        summed = lax.dot_general(
            sum_map, ret[...].reshape(experts * cap, slab), (((0,), (0,)), ((), ())),
            preferred_element_type=F32,
        )
        spread(1, out_r, summed.astype(BF16))
        spread_on(1, out_r)
        spread_end(0, out_m)
        spread_end(1, out_r)
        for copy in sent:
            copy.wait_send()

    edge = 16 * -(-(taps_n - 1) // 16)
    dma = pltpu.SemaphoreType.DMA
    far = max(1, high - 1)
    v = lambda shape: pltpu.VMEM(shape, BF16)

    def scratch(hid):
        return [
            v((width, chan)), v((width, chan)), v((width, chan)), v((chan, width)),
            v((width, hid)), v((width, hid)), v((hid, width)),
            v((high, experts, cap, slab)), v((groups, steps, per, cap, slab)),
            v((steps, CORES, high, rows, slab)), v((steps, high, rows, slab)),
            v((steps, high, rows, slab)), v((steps, far, rows, slab)),
            v((steps, per, cap, slab)), v((experts, cap, slab)),
            v((edge, chan)), v((edge, chan)),
            v((CORES, high, mrows, slab)), v((high, mrows, slab)), v((high, mrows, slab)),
            v((far, mrows, slab)),
            dma((7,)), dma((high,)),
            dma((steps, per, high)), dma((steps, per, high)), dma((steps, far)), dma((steps, far)),
            dma((steps, high)), dma((steps, high)), dma((steps + 1,)), dma((steps + 1,)),
            dma((steps + 1, far)), dma((steps + 1, far)), dma((steps, per)), dma((experts,)),
            dma((1,)), dma((1,)), dma((2, far)), dma((2, far)), dma((2, high)), dma((2, high)),
        ]

    return kernel, scratch


def on_device(
    mixer_rows, mixer_gain, inner_weight, gate_in_weight, gate_out_weight, conv_taps,
    mixer_out_weight, routed_rows, routed_gain, route_ids, route_weights,
    expert_gate, expert_up, expert_down,
):
    experts, groups = lax.axis_size("ep"), lax.axis_size("tp")
    tok, picks = route_ids.shape
    width = routed_rows.shape[1]
    cap = 2 * tok * picks // experts
    per = max(1, min(experts, tok // cap))
    steps = experts // per
    mrows = mixer_rows.shape[0]
    taps_n, chan = conv_taps.shape
    kernel, scratch = make_kernel(
        experts, groups, tok, picks, width, cap, steps, per, mrows, taps_n, chan
    )
    near, far = pl.BlockSpec(memory_space=pltpu.VMEM), pl.BlockSpec(memory_space=pl.ANY)
    return pl.pallas_call(
        kernel,
        out_shape=(
            jax.ShapeDtypeStruct(mixer_rows.shape, BF16),
            jax.ShapeDtypeStruct(routed_rows.shape, BF16),
        ),
        in_specs=[near, near, far, far, far, near, far, near, near, near, near, far, far, far],
        out_specs=(near, near),
        scratch_shapes=scratch(expert_gate.shape[2]),
        compiler_params=pltpu.CompilerParams(
            collective_id=0, has_side_effects=True, vmem_limit_bytes=60 * 1024 * 1024
        ),
        name="mixer_and_experts",
    )(
        mixer_rows, mixer_gain[None, :], inner_weight, gate_in_weight, gate_out_weight, conv_taps,
        mixer_out_weight, routed_rows, routed_gain[None, :], route_ids.T, route_weights.T,
        expert_gate[0], expert_up[0], expert_down[0],
    )


def solution(mesh):
    return jax.shard_map(
        on_device,
        mesh=mesh,
        in_specs=(
            P("ep", None), P(), P(None, "tp"), P(None, "tp"), P(None, "tp"), P(None, "tp"),
            P("tp", None), P("ep", None), P(), P("ep", None), P("ep", None),
            P("ep", None, "tp"), P("ep", None, "tp"), P("ep", "tp", None),
        ),
        out_specs=(P("ep", None), P("ep", None)),
        check_vma=False,
    )
```
